512 devices in a mesh: sp: 64 (over z, y), tp: 8 (over x, core).
Axes of the slice: x: 4, y: 4, z: 16, core: 2. Of those that a mesh axis runs over, the one named last changes fastest.
Arguments:
- residual: bfloat16 [8192, 2048], P('sp'), may hold values from -6 to 6
- query_first: bfloat16 [8192, 8, 128], P('sp', 'tp'), may hold values from -6.5 to 6.5
- key_first: bfloat16 [8192, 8, 128], P('sp', 'tp'), may hold values from -6.5 to 6.5
- value_first: bfloat16 [8192, 8, 128], P('sp', 'tp'), may hold values from -6 to 6
- query_second: bfloat16 [8192, 8, 64], P('sp', 'tp'), may hold values from -6.5 to 6.5
- key_second: bfloat16 [8192, 8, 64], P('sp', 'tp'), may hold values from -6.5 to 6.5
- value_second: bfloat16 [8192, 8, 64], P('sp', 'tp'), may hold values from -6 to 6
- balance_first: float32 [8], P('tp'), may hold values from 0.3 to 0.8
- balance_second: float32 [8], P('tp'), may hold values from 0.3 to 0.8
- head_gain_first: float32 [128], replicated, may hold values from 0.1 to 1.9
- head_gain_second: float32 [64], replicated, may hold values from 0.1 to 1.9
- out_first: bfloat16 [1024, 2048], P('tp'), may hold values from -0.15625 to 0.15625
- out_second: bfloat16 [512, 2048], P('tp'), may hold values from -0.15625 to 0.15625
- mlp_gain: float32 [2048], replicated, may hold values from 0.1 to 1.9
- up_weight: bfloat16 [2048, 8192], P('sp', 'tp'), may hold values from -0.125 to 0.125
- down_weight: bfloat16 [2048, 8192], P('sp', 'tp'), may hold values from -0.0625 to 0.0625
Outputs:
- layer_out: bfloat16 [8192, 2048], P('sp')
The draws below stay inside these ranges and needn't reach their ends.
All inputs are finite; a program needn't handle non-finite values.
Results may differ from the reference program's by a relative error of at most 0.018.
Values may be sent and summed in bfloat16 or wider, within the bound.
A program may use at most 64 MiB of HBM per device.

```python
import math
import jax
import jax.numpy as jnp
from jax import lax

D = 2048
FF = 8192
HEADS_A = 8
HEADS_B = 8
DK_A = 64
DV_A = 128
DK_B = 32
DV_B = 64
SEQ = 8192
N_TP = 8


def drawn(key, heads, head_size):
    width = 2 * head_size
    queries = jnp.clip(1.3 * jax.random.normal(jax.random.fold_in(key, 11), (SEQ, heads, width), jnp.float32), -6.5, 6.5)
    keys = jnp.clip(1.3 * jax.random.normal(jax.random.fold_in(key, 12), (SEQ, heads, width), jnp.float32), -6.5, 6.5)
    return (queries, keys)


def draw_query_first(key, part):
    return drawn(jax.random.fold_in(key, 1), HEADS_A, DK_A)[0].astype(jnp.bfloat16)


def draw_key_first(key, part):
    return drawn(jax.random.fold_in(key, 1), HEADS_A, DK_A)[1].astype(jnp.bfloat16)


def draw_query_second(key, part):
    return drawn(jax.random.fold_in(key, 2), HEADS_B, DK_B)[0].astype(jnp.bfloat16)


def draw_key_second(key, part):
    return drawn(jax.random.fold_in(key, 2), HEADS_B, DK_B)[1].astype(jnp.bfloat16)


def block_scale(key, dims, shards, smallest, high):
    loudness = 1.0
    for position, parts in shards:
        draws = jax.random.uniform(jax.random.fold_in(jax.random.fold_in(key, 6), position), (parts,), jnp.float32, smallest / len(shards), high / len(shards))
        loudness = loudness * jnp.repeat(jnp.exp(draws), dims[position] // parts).reshape((-1,) + (1,) * (len(dims) - 1 - position))
    return loudness


def gaussian(rng, shape, spread, limit, split=(), kind=jnp.bfloat16):
    values = spread * jax.random.normal(rng, shape, jnp.float32)
    if split:
        values = values * block_scale(rng, shape, split, -0.22, 0.18)
    return jnp.clip(values, -limit, limit).astype(kind)


def setup_inputs(seed: int = 0) -> dict:
    key_list = jax.random.split(jax.random.key(seed), 17)
    return {
        "residual": gaussian(key_list[0], (SEQ, D), 1.0, 6.0, ((0, 64),)),
        "query_first": draw_query_first(jax.random.fold_in(key_list[16], 71), 0),
        "key_first": draw_key_first(jax.random.fold_in(key_list[16], 71), 0),
        "value_first": gaussian(key_list[3], (SEQ, HEADS_A, DV_A), 1.0, 6.0, ((0, 64), (1, 8))),
        "query_second": draw_query_second(jax.random.fold_in(key_list[16], 71), 0),
        "key_second": draw_key_second(jax.random.fold_in(key_list[16], 71), 0),
        "value_second": gaussian(key_list[6], (SEQ, HEADS_B, DV_B), 1.0, 6.0, ((0, 64), (1, 8))),
        "balance_first": jnp.clip(0.3 + 0.5 * jax.random.uniform(key_list[7], (HEADS_A,), jnp.float32) ** block_scale(key_list[7], (HEADS_A,), ((0, 8),), -0.2, 0.2), 0.3, 0.8),
        "balance_second": jnp.clip(0.3 + 0.5 * jax.random.uniform(key_list[8], (HEADS_B,), jnp.float32) ** block_scale(key_list[8], (HEADS_B,), ((0, 8),), -0.2, 0.2), 0.3, 0.8),
        "head_gain_first": jnp.clip(1.0 + 0.18 * jax.random.normal(key_list[9], (DV_A,), jnp.float32), 0.1, 1.9),
        "head_gain_second": jnp.clip(1.0 + 0.18 * jax.random.normal(key_list[10], (DV_B,), jnp.float32), 0.1, 1.9),
        "out_first": gaussian(key_list[11], (HEADS_A * DV_A, D), (HEADS_A * DV_A + HEADS_B * DV_B) ** -0.5, 0.15625, ((0, 8),)),
        "out_second": gaussian(key_list[12], (HEADS_B * DV_B, D), (HEADS_A * DV_A + HEADS_B * DV_B) ** -0.5, 0.15625, ((0, 8),)),
        "mlp_gain": jnp.clip(1.0 + 0.18 * jax.random.normal(key_list[13], (D,), jnp.float32), 0.1, 1.9),
        "up_weight": gaussian(key_list[14], (D, FF), D ** -0.5, 0.125, ((0, 64), (1, 8))),
        "down_weight": gaussian(key_list[15], (D, FF), FF ** -0.5, 0.0625, ((0, 64), (1, 8))),
    }


EPSILON = 1e-06
HEAD_SCALE = 0.8

def group_heads(queries, keys, values, balance, gain, head_size):
    seq = queries.shape[0]
    heads = queries.shape[1]
    depth = values.shape[2]
    block = math.gcd(256, seq)
    count = seq // block
    query_maps = queries.astype(jnp.float32).reshape(count, block, heads, 2, head_size)
    key_maps = keys.astype(jnp.float32).reshape(seq, heads, 2, head_size)
    value_float = values.astype(jnp.float32)
    columns = jnp.arange(seq, dtype=jnp.int32)
    gain_float = gain.astype(jnp.float32)

    def one_block(args):
        query_block, start = args
        scores = jnp.einsum('qhmd,khmd->hmqk', query_block, key_maps) * head_size ** (-0.5)
        positions = start + jnp.arange(block, dtype=jnp.int32)
        scores = jnp.where(columns[None, :] <= positions[:, None], scores, -jnp.inf)
        probs = jax.nn.softmax(scores, axis=-1)
        mixed = (probs[:, 0] - balance[:, None, None] * probs[:, 1]).astype(jnp.bfloat16)
        mixed = lax.optimization_barrier(mixed).astype(jnp.float32)
        summed = jnp.einsum('hqk,khe->qhe', mixed, value_float)
        power = lax.optimization_barrier(jnp.mean(summed * summed, axis=-1, keepdims=True))
        normed = summed * lax.rsqrt(power + EPSILON) * gain_float * HEAD_SCALE
        return normed.astype(jnp.bfloat16)
    starts = jnp.arange(count, dtype=jnp.int32) * block
    result = lax.map(one_block, (query_maps, starts))
    return result.reshape(seq, heads * depth)

def reference(residual, query_first, key_first, value_first, query_second, key_second, value_second, balance_first, balance_second, head_gain_first, head_gain_second, out_first, out_second, mlp_gain, up_weight, down_weight):
    heads_first = group_heads(query_first, key_first, value_first, balance_first, head_gain_first, DK_A)
    heads_second = group_heads(query_second, key_second, value_second, balance_second, head_gain_second, DK_B)
    seq = residual.shape[0]
    width = residual.shape[1]
    width_first = heads_first.shape[1] // N_TP
    width_second = heads_second.shape[1] // N_TP

    def head_part(number, total):
        offset_first = (number * width_first).astype(jnp.int32)
        offset_second = (number * width_second).astype(jnp.int32)
        part = jnp.dot(lax.dynamic_slice_in_dim(heads_first, offset_first, width_first, 1), lax.dynamic_slice_in_dim(out_first, offset_first, width_first, 0), preferred_element_type=jnp.float32)
        part = part + jnp.dot(lax.dynamic_slice_in_dim(heads_second, offset_second, width_second, 1), lax.dynamic_slice_in_dim(out_second, offset_second, width_second, 0), preferred_element_type=jnp.float32)
        rounded = lax.optimization_barrier(part.astype(jnp.bfloat16))
        return total + rounded.astype(jnp.float32)
    head_total = lax.fori_loop(0, N_TP, head_part, jnp.zeros((seq, width), jnp.float32))
    mixed = (residual.astype(jnp.float32) + head_total).astype(jnp.bfloat16)
    mixed_float = mixed.astype(jnp.float32)
    power = lax.optimization_barrier(jnp.mean(mixed_float * mixed_float, axis=-1, keepdims=True))
    normed = (mixed_float * lax.rsqrt(power + EPSILON) * mlp_gain.astype(jnp.float32)).astype(jnp.bfloat16)
    lifted = jnp.dot(normed, up_weight, preferred_element_type=jnp.float32)
    active = jax.nn.relu(lifted)
    hidden = (active * active).astype(jnp.bfloat16)
    width_hidden = hidden.shape[1] // N_TP

    def down_part(number, total):
        offset = (number * width_hidden).astype(jnp.int32)
        part = lax.dot_general(lax.dynamic_slice_in_dim(hidden, offset, width_hidden, 1), lax.dynamic_slice_in_dim(down_weight, offset, width_hidden, 1), (((1,), (1,)), ((), ())), preferred_element_type=jnp.float32)
        rounded = lax.optimization_barrier(part.astype(jnp.bfloat16))
        return total + rounded.astype(jnp.float32)
    down_total = lax.fori_loop(0, N_TP, down_part, jnp.zeros((seq, width), jnp.float32))
    return (mixed_float + down_total).astype(jnp.bfloat16)
```

```python
import functools
import math

import jax
import jax.numpy as jnp
from jax import lax
from jax.experimental import pallas as pl
from jax.experimental.pallas import tpu as pltpu
from jax.sharding import PartitionSpec as P

MESH = pl.DeviceIdType.MESH
DK_A = 64
DK_B = 32
EPSILON = 1e-06
HEAD_SCALE = 0.8
NY = 4
NX = 4
ROWS = 128
BLOCK = NY * ROWS
D = 2048
FB = 256
NB = D // FB
LOW = -1e30
RATES = tuple(k**-0.5 * math.log2(math.e) for k in (DK_A, DK_A, DK_B, DK_B))
SPANS = ((0, 128), (128, 256), (256, 320), (320, 384))
F32 = jnp.float32
BF16 = jnp.bfloat16


def nt(a, b):
    return lax.dot_general(a, b, (((1,), (1,)), ((), ())), preferred_element_type=F32)


def kernel(
    nz,
    qkv,
    balances,
    gains,
    mlp_gain,
    residual,
    out_first,
    out_second,
    up,
    down,
    out,
    qbuf,
    qpad,
    kv,
    acc,
    stats,
    xsnd,
    xacc,
    xstats,
    hx,
    hmat,
    wo,
    res,
    wup,
    wdn,
    pb,
    rb,
    mx,
    gb,
    db,
    rd,
    sb,
    rs,
    loc,
    qs,
    qr,
    ks,
    kr,
    ys,
    yr,
    ws,
    wr,
    vs,
    vr,
    os,
    orr,
    xs,
    xr,
    hs,
    hr,
    ps,
    pr,
    dsm,
    drm,
    ss,
    sr,
    fs,
    fr,
    gs,
    gr,
):
    sp = lax.axis_index("sp")
    tp = lax.axis_index("tp")
    z, y = sp // NY, sp % NY
    x, c = tp // 2, tp % 2

    def near(dy, dx):
        return (z * NY + (y + dy) % NY, ((x + dx) % NX) * 2 + c)

    partner = (sp, x * 2 + (1 - c))
    above = (((z + 1) % nz) * NY + y, tp)
    below = (((z + nz - 1) % nz) * NY + y, tp)
    others = [(dy, dx) for dy in range(NY) for dx in range(NX) if dy or dx]

    def send(src, dst, ssem, rsem, device):
        return pltpu.make_async_remote_copy(
            src_ref=src,
            dst_ref=dst,
            send_sem=ssem,
            recv_sem=rsem,
            device_id=device,
            device_id_type=MESH,
        )

    def arrive(ref, ssem, rsem):
        send(ref, ref, ssem, rsem, partner).wait_recv()

    def left(ref, ssem, rsem):
        send(ref, ref, ssem, rsem, partner).wait_send()

    barrier = pltpu.get_barrier_semaphore()
    for device in [near(dy, dx) for dy, dx in others] + [partner, above, below]:
        pl.semaphore_signal(barrier, inc=1, device_id=device, device_id_type=MESH)

    kv[z, 0] = qkv[2]
    kv[z, 1] = qkv[3].astype(F32).T.astype(BF16)
    kv[z, 2] = qkv[4]
    qbuf[y, 0] = qkv[0]
    qbuf[y, 1] = qkv[1]
    pl.semaphore_wait(barrier, len(others) + 3)

    for ch in range(3):
        for way, device in ((0, above), (1, below)):
            send(
                kv.at[z, ch], kv.at[z, ch], ks.at[way, 0, ch], kr.at[way, 0, ch], device
            ).start()
    for d in range(1, NY):
        send(qkv.at[pl.ds(0, 2)], qbuf.at[y], qs.at[d - 1], qr.at[d - 1], near(d, 0)).start()

    own = pl.ds(pl.multiple_of(z * ROWS + y * 32, 32), 32)
    mine = pl.ds(pl.multiple_of(y * FB, FB), FB)
    tok = pl.ds(pl.multiple_of(y * ROWS, ROWS), ROWS)
    ra = pl.ds(pl.multiple_of(x * 128, 128), 128)
    rbw = pl.ds(pl.multiple_of(512 + x * 64, 64), 64)
    locals_ = [
        pltpu.make_async_copy(up.at[:, mine], wup.at[own], loc.at[0]),
        pltpu.make_async_copy(down.at[:, mine], wdn.at[own], loc.at[1]),
        pltpu.make_async_copy(residual, res.at[tok], loc.at[2]),
        pltpu.make_async_copy(out_first, wo.at[ra], loc.at[3]),
        pltpu.make_async_copy(out_second, wo.at[rbw], loc.at[4]),
    ]
    for copy in locals_:
        copy.start()
    for d in range(1, NY):
        part = pl.ds(pl.multiple_of(((y + d) % NY) * FB, FB), FB)
        send(up.at[:, part], wup.at[own], ys.at[d - 1, 0], yr.at[d - 1, 0], near(d, 0)).start()
        send(down.at[:, part], wdn.at[own], ys.at[d - 1, 1], yr.at[d - 1, 1], near(d, 0)).start()
    for d in range(1, NX):
        send(out_first, wo.at[ra], os.at[d - 1, 0], orr.at[d - 1, 0], near(0, d)).start()
        send(out_second, wo.at[rbw], os.at[d - 1, 1], orr.at[d - 1, 1], near(0, d)).start()
    for d in range(1, NY):
        send(residual, res.at[tok], vs.at[d - 1], vr.at[d - 1], near(d, 0)).start()

    stats[pl.ds(0, 4)] = jnp.full((4, BLOCK), LOW, F32)
    stats[pl.ds(4, 4)] = jnp.zeros((4, BLOCK), F32)
    acc[...] = jnp.zeros_like(acc)

    for d in range(1, NY):
        arrive(qbuf.at[(y + NY - d) % NY], qs.at[d - 1], qr.at[d - 1])
    lane = lax.broadcasted_iota(jnp.int32, (ROWS, 128), 1)
    bounds = ((0, 0, 64), (0, 64, 128), (1, 0, 32), (1, 32, 64))
    for i, (g, low, high) in enumerate(bounds):
        keep = ((lane >= low) & (lane < high)).astype(F32).astype(BF16)
        for j in range(NY):
            qpad[i, pl.ds(j * ROWS, ROWS)] = qbuf[j, g] * keep

    def attend(slot, masked):
        both = kv[slot, 2].astype(F32).T.astype(BF16)
        for i in range(4):
            keys = kv[slot, 0] if i < 2 else kv[slot, 2]
            values = kv[slot, 1] if i < 2 else both[64:128]
            lo, hi = SPANS[i]
            for half in range(2):
                cols = pl.ds(half * 256, 256)
                s = nt(keys, qpad[i, cols])
                if masked:
                    kpos = y * ROWS + lax.broadcasted_iota(jnp.int32, s.shape, 0)
                    qpos = half * 256 + lax.broadcasted_iota(jnp.int32, s.shape, 1)
                    visible = kpos <= qpos
                    s = jnp.where(visible, s, LOW)
                old = stats[pl.ds(i, 1), cols]
                new = jnp.maximum(old, jnp.max(s, axis=0, keepdims=True))
                p = jnp.exp2((s - new) * RATES[i])
                if masked:
                    p = jnp.where(visible, p, 0.0)
                alpha = jnp.exp2((old - new) * RATES[i])
                stats[pl.ds(i, 1), cols] = new
                stats[pl.ds(4 + i, 1), cols] = stats[pl.ds(4 + i, 1), cols] * alpha + jnp.sum(
                    p, axis=0, keepdims=True
                )
                rows = pl.ds(lo, hi - lo)
                acc[rows, cols] = acc[rows, cols] * alpha + jnp.dot(
                    values, p.astype(BF16), preferred_element_type=F32
                )

    attend(z, True)

    def ring(k, _):
        upper = lax.rem(z - (k + 1) + nz, nz)
        lower = lax.rem(z + k + 1, nz)
        for ch in range(3):
            arrive(kv.at[upper, ch], ks.at[0, k, ch], kr.at[0, k, ch])

            @pl.when(k < nz // 2 - 1)
            def _():
                ref = kv.at[upper, ch]
                send(ref, ref, ks.at[0, k + 1, ch], kr.at[0, k + 1, ch], above).start()
                arrive(kv.at[lower, ch], ks.at[1, k, ch], kr.at[1, k, ch])

            @pl.when(k < nz // 2 - 2)
            def _():
                ref = kv.at[lower, ch]
                send(ref, ref, ks.at[1, k + 1, ch], kr.at[1, k + 1, ch], below).start()

        def side(way, _):
            slot = jnp.where(way == 0, upper, lower)
            first = (way == 0) & (k + 1 <= z)
            second = (way == 1) & (z + k + 1 >= nz) & (k < nz // 2 - 1)

            @pl.when(first | second)
            def _():
                attend(slot, False)

            return 0

        lax.fori_loop(0, 2, side, 0)
        return 0

    lax.fori_loop(0, nz // 2, ring, 0)

    def shard(ref, at):
        return ref.at[pl.ds(pl.multiple_of(at * ROWS, ROWS), ROWS)]

    for copy in locals_:
        copy.wait()
    for d in range(1, NY):
        rows = pl.ds(pl.multiple_of(z * ROWS + ((y + NY - d) % NY) * 32, 32), 32)
        for i, w in enumerate((wup, wdn)):
            arrive(w.at[rows], ys.at[d - 1, i], yr.at[d - 1, i])
    for i, w in enumerate((wup, wdn)):
        for way, device in ((0, above), (1, below)):
            send(shard(w, z), shard(w, z), ws.at[way, 0, i], wr.at[way, 0, i], device).start()

    def turn(k):
        upper = lax.rem(z - (k + 1) + nz, nz)
        lower = lax.rem(z + k + 1, nz)
        for i, w in enumerate((wup, wdn)):
            ref = shard(w, upper)
            arrive(ref, ws.at[0, k, i], wr.at[0, k, i])
            if k < nz // 2 - 1:
                send(ref, ref, ws.at[0, k + 1, i], wr.at[0, k + 1, i], above).start()
                ref = shard(w, lower)
                arrive(ref, ws.at[1, k, i], wr.at[1, k, i])
                if k < nz // 2 - 2:
                    send(ref, ref, ws.at[1, k + 1, i], wr.at[1, k + 1, i], below).start()

    turns = list(range(nz // 2))

    def turn_some(count):
        for k in turns[:count]:
            turn(k)
        del turns[:count]

    turn_some(0)
    for j in range(NY):
        xsnd[j] = acc[:, pl.ds(j * ROWS, ROWS)].astype(BF16)
    for d in range(1, NY):
        there = (y + d) % NY
        part = stats.at[:, pl.ds(pl.multiple_of(there * ROWS, ROWS), ROWS)]
        send(xsnd.at[there], xacc.at[y], xs.at[d - 1, 0], xr.at[d - 1, 0], near(d, 0)).start()
        send(part, xstats.at[y], xs.at[d - 1, 1], xr.at[d - 1, 1], near(d, 0)).start()
    xacc[y] = xsnd[y]
    xstats[y] = stats[:, tok]
    turn_some(1)
    for d in range(1, NY):
        there = (y + NY - d) % NY
        arrive(xacc.at[there], xs.at[d - 1, 0], xr.at[d - 1, 0])
        arrive(xstats.at[there], xs.at[d - 1, 1], xr.at[d - 1, 1])

    maps = []
    for i in range(4):
        lo, hi = SPANS[i]
        tops = [xstats[j, i : i + 1] for j in range(NY)]
        top = functools.reduce(jnp.maximum, tops)
        shares = [jnp.exp2((t - top) * RATES[i]) for t in tops]
        total = sum(w * xstats[j, 4 + i : 5 + i] for j, w in enumerate(shares))
        maps.append(
            sum(
                xacc[j, pl.ds(lo, hi - lo)].astype(F32) * (w / total)
                for j, w in enumerate(shares)
            )
        )
    for g in range(2):
        mixed = maps[2 * g] - balances[g] * maps[2 * g + 1]
        size = mixed.shape[0]
        power = jnp.mean(mixed * mixed, axis=0, keepdims=True)
        gain = jnp.broadcast_to(gains[g : g + 1], (128, 128)).T[0:size]
        normed = mixed * lax.rsqrt(power + EPSILON) * gain * HEAD_SCALE
        hx[y, x, pl.ds(128 * g, size)] = normed.astype(BF16)
    for n, (dy, dx) in enumerate(others):
        send(hx.at[y, x], hx.at[y, x], hs.at[n], hr.at[n], near(dy, dx)).start()
    turn_some(3)
    for d in range(1, NX):
        there = (x + NX - d) % NX
        for i, (size, base) in enumerate(((128, 0), (64, 512))):
            ref = wo.at[pl.ds(pl.multiple_of(base + there * size, size), size)]
            arrive(ref, os.at[d - 1, i], orr.at[d - 1, i])
    for n, (dy, dx) in enumerate(others):
        ref = hx.at[(y + NY - dy) % NY, (x + NX - dx) % NX]
        arrive(ref, hs.at[n], hr.at[n])
    for j in range(NY):
        rows = pl.ds(j * ROWS, ROWS)
        for i in range(NX):
            hmat[rows, pl.ds(i * 128, 128)] = hx[j, i, pl.ds(0, 128)].astype(F32).T.astype(BF16)
        for i in range(NX // 2):
            pair = jnp.concatenate(
                [hx[j, 2 * i, pl.ds(128, 64)], hx[j, 2 * i + 1, pl.ds(128, 64)]], axis=0
            )
            hmat[rows, pl.ds(512 + i * 128, 128)] = pair.astype(F32).T.astype(BF16)

    def block(n):
        return pl.ds(pl.multiple_of(n * FB, FB), FB)

    def project(n, _):
        pb[n] = jnp.dot(hmat[...], wo[:, block(n)], preferred_element_type=F32).astype(BF16)
        send(pb.at[n], rb.at[n], ps.at[n], pr.at[n], partner).start()
        return 0

    lax.fori_loop(0, NB, project, 0)
    for d in range(1, NY):
        there = pl.ds(pl.multiple_of(((y + NY - d) % NY) * ROWS, ROWS), ROWS)
        arrive(res.at[there], vs.at[d - 1], vr.at[d - 1])
    turn_some(2)

    def mix(n, power):
        arrive(rb.at[n], ps.at[n], pr.at[n])
        cols = block(n)
        mixed = (
            res[:, cols].astype(F32) + (pb[n].astype(F32) + rb[n].astype(F32))
        ).astype(BF16)
        mx[:, cols] = mixed
        wide = mixed.astype(F32)
        gb[:, cols] = (wide * mlp_gain[:, cols]).astype(BF16)
        square = wide * wide
        return power + (square[:, 0:128] + square[:, 128:256])

    power = lax.fori_loop(0, NB, mix, jnp.zeros((BLOCK, 128), F32))
    scale = lax.rsqrt(jnp.sum(power, axis=-1, keepdims=True) * (1.0 / D) + EPSILON)
    turn_some(len(turns))
    lifted = jnp.dot(gb[...], wup[...], preferred_element_type=F32) * scale
    active = jnp.maximum(lifted, 0.0)
    gb[:, pl.ds(0, FB)] = (active * active).astype(BF16)

    def lower_part(n, _):
        rows = pl.ds(pl.multiple_of(n * FB, FB), FB)
        term = nt(gb[:, pl.ds(0, FB)], wdn[rows]).astype(BF16)
        for j in range(NY):
            for h in range(2):
                at = j * ROWS + h * 64
                db[n, h, pl.ds(j * 64, 64)] = term[at : at + 64]
        send(db.at[n, 1 - c], rd.at[n], dsm.at[n], drm.at[n], partner).start()
        return 0

    lax.fori_loop(0, NB, lower_part, 0)

    def gather(n, _):
        arrive(rd.at[n], dsm.at[n], drm.at[n])
        both = (db[n, c].astype(F32) + rd[n].astype(F32)).astype(BF16)
        cols = block(n)
        for j in range(16):
            sb[j, :, cols] = both[j * 16 : j * 16 + 16]
        return 0

    lax.fori_loop(0, NB, gather, 0)
    for n, (dy, dx) in enumerate(others):
        to = ((y + dy) % NY) * NX + (x + dx) % NX
        send(sb.at[to], rs.at[y * NX + x], ss.at[n], sr.at[n], near(dy, dx)).start()
    rs[y * NX + x] = sb[y * NX + x]
    for n, (dy, dx) in enumerate(others):
        ref = rs.at[((y + NY - dy) % NY) * NX + (x + NX - dx) % NX]
        arrive(ref, ss.at[n], sr.at[n])

    def final(n, _):
        cols = block(n)
        added = rs[:, :, cols].astype(F32).sum(axis=0)
        base = mx[pl.ds(pl.multiple_of(y * ROWS + c * 64 + x * 16, 16), 16), cols].astype(F32)
        out[pl.ds(pl.multiple_of(c * 64 + x * 16, 16), 16), cols] = (base + added).astype(BF16)
        return 0

    lax.fori_loop(0, NB, final, 0)

    def piece(core, at):
        return out.at[pl.ds(pl.multiple_of(core * 64 + at * 16, 16), 16)]

    send(piece(c, x), piece(c, x), gs.at[0], gr.at[0], partner).start()
    for d in range(1, NX):
        send(piece(c, x), piece(c, x), fs.at[d - 1], fr.at[d - 1], near(0, d)).start()
    for d in range(1, NX):
        ref = piece(c, (x + NX - d) % NX)
        arrive(ref, fs.at[d - 1], fr.at[d - 1])
        send(ref, ref, gs.at[d], gr.at[d], partner).start()
    for d in range(NX):
        arrive(piece(1 - c, (x + NX - d) % NX), gs.at[d], gr.at[d])

    for d in range(NX - 1):
        left(piece(c, x), fs.at[d], fr.at[d])
        left(out_first, os.at[d, 0], orr.at[d, 0])
        left(out_second, os.at[d, 1], orr.at[d, 1])
    for d in range(NX):
        left(piece(c, x), gs.at[d], gr.at[d])
    for d in range(NY - 1):
        left(qbuf.at[0], qs.at[d], qr.at[d])
        left(up.at[:, mine], ys.at[d, 0], yr.at[d, 0])
        left(down.at[:, mine], ys.at[d, 1], yr.at[d, 1])
        left(residual, vs.at[d], vr.at[d])
        left(xsnd.at[0], xs.at[d, 0], xr.at[d, 0])
        left(xstats.at[0], xs.at[d, 1], xr.at[d, 1])
    for n in range(len(others)):
        left(hx.at[0, 0], hs.at[n], hr.at[n])
        left(sb.at[0], ss.at[n], sr.at[n])
    for n in range(NB):
        left(pb.at[0], ps.at[n], pr.at[n])
        left(rd.at[0], dsm.at[n], drm.at[n])
    for way, steps in ((0, nz // 2), (1, nz // 2 - 1)):
        for k in range(steps):
            for ch in range(3):
                left(kv.at[0, ch], ks.at[way, k, ch], kr.at[way, k, ch])
            for i in range(2):
                left(shard(wup, 0), ws.at[way, k, i], wr.at[way, k, i])


def layer(
    residual,
    query_first,
    key_first,
    value_first,
    query_second,
    key_second,
    value_second,
    balance_first,
    balance_second,
    head_gain_first,
    head_gain_second,
    out_first,
    out_second,
    mlp_gain,
    up_weight,
    down_weight,
):
    nz = lax.axis_size("sp") // NY
    flat = lambda a: a.reshape(a.shape[0], a.shape[2])
    query_low, key_low, value_low = flat(query_second), flat(key_second), flat(value_second)
    qkv = jnp.stack(
        [
            flat(query_first),
            jnp.concatenate([query_low, jnp.zeros_like(query_low)], axis=1),
            flat(key_first),
            flat(value_first),
            jnp.concatenate([key_low, value_low], axis=1),
        ]
    )
    balances = jnp.concatenate([balance_first, balance_second])
    gains = jnp.stack([head_gain_first, jnp.concatenate([head_gain_second, head_gain_second])])
    vmem = pl.BlockSpec(memory_space=pltpu.VMEM)
    smem = pl.BlockSpec(memory_space=pltpu.SMEM)
    anywhere = pl.BlockSpec(memory_space=pl.ANY)
    half = nz // 2
    dma = lambda *shape: pltpu.SemaphoreType.DMA(shape)
    return pl.pallas_call(
        functools.partial(kernel, nz),
        out_shape=jax.ShapeDtypeStruct((ROWS, D), BF16),
        in_specs=[vmem, smem, vmem, vmem] + [anywhere] * 5,
        out_specs=vmem,
        scratch_shapes=[
            pltpu.VMEM((NY, 2, ROWS, 128), BF16),
            pltpu.VMEM((4, BLOCK, 128), BF16),
            pltpu.VMEM((nz, 3, ROWS, 128), BF16),
            pltpu.VMEM((384, BLOCK), F32),
            pltpu.VMEM((8, BLOCK), F32),
            pltpu.VMEM((NY, 384, ROWS), BF16),
            pltpu.VMEM((NY, 384, ROWS), BF16),
            pltpu.VMEM((NY, 8, ROWS), F32),
            pltpu.VMEM((NY, NX, 192, ROWS), BF16),
            pltpu.VMEM((BLOCK, 768), BF16),
            pltpu.VMEM((768, D), BF16),
            pltpu.VMEM((BLOCK, D), BF16),
            pltpu.VMEM((nz * ROWS, FB), BF16),
            pltpu.VMEM((nz * ROWS, FB), BF16),
            pltpu.VMEM((NB, BLOCK, FB), BF16),
            pltpu.VMEM((NB, BLOCK, FB), BF16),
            pltpu.VMEM((BLOCK, D), BF16),
            pltpu.VMEM((BLOCK, D), BF16),
            pltpu.VMEM((NB, 2, BLOCK // 2, FB), BF16),
            pltpu.VMEM((NB, BLOCK // 2, FB), BF16),
            pltpu.VMEM((16, 16, D), BF16),
            pltpu.VMEM((16, 16, D), BF16),
            dma(5),
            dma(3),
            dma(3),
            dma(2, half, 3),
            dma(2, half, 3),
            dma(3, 2),
            dma(3, 2),
            dma(2, half, 2),
            dma(2, half, 2),
            dma(3),
            dma(3),
            dma(3, 2),
            dma(3, 2),
            dma(3, 2),
            dma(3, 2),
            dma(15),
            dma(15),
            dma(NB),
            dma(NB),
            dma(NB),
            dma(NB),
            dma(15),
            dma(15),
            dma(3),
            dma(3),
            dma(4),
            dma(4),
        ],
        compiler_params=pltpu.CompilerParams(
            collective_id=0, has_side_effects=True, vmem_limit_bytes=60 * 1024 * 1024
        ),
    )(
        qkv,
        balances,
        gains,
        mlp_gain.reshape(1, D),
        residual,
        out_first,
        out_second,
        up_weight,
        down_weight,
    )


def solution(mesh):
    heads = P("sp", "tp", None)
    whole = P("sp", "tp")
    in_specs = (
        P("sp", None),
        *([heads] * 6),
        P("tp"),
        P("tp"),
        P(),
        P(),
        P("tp", None),
        P("tp", None),
        P(),
        whole,
        whole,
    )
    return jax.shard_map(
        layer, mesh=mesh, in_specs=in_specs, out_specs=P("sp", None), check_vma=False
    )
```

```python
import functools
import math

import jax
import jax.numpy as jnp
from jax import lax
from jax.experimental import pallas as pl
from jax.experimental.pallas import tpu as pltpu
from jax.sharding import PartitionSpec as P

MESH = pl.DeviceIdType.MESH
DK_A = 64
DK_B = 32
EPSILON = 1e-06
HEAD_SCALE = 0.8
NY = 4
NX = 4
ROWS = 128
BLOCK = NY * ROWS
D = 2048
FB = 256
NB = D // FB
LOW = -1e30
EARLY = 5
TURNS = (2, 3)
RATES = tuple(k**-0.5 * math.log2(math.e) for k in (DK_A, DK_A, DK_B, DK_B))
SPANS = ((0, 128), (128, 256), (256, 320), (320, 384))
F32 = jnp.float32
BF16 = jnp.bfloat16


def nt(a, b):
    return lax.dot_general(a, b, (((1,), (1,)), ((), ())), preferred_element_type=F32)


def kernel(
    nz,
    balance_a,
    balance_b,
    query_a,
    key_a,
    value_a,
    query_b,
    key_b,
    value_b,
    gain_a,
    gain_b,
    mlp_gain,
    residual,
    out_first,
    out_second,
    up,
    down,
    out,
    qa,
    qb,
    vraw,
    ga,
    gbb,
    bal,
    mgain,
    qpad,
    kv,
    acc,
    stats,
    xsnd,
    xacc,
    xstats,
    hx,
    hmat,
    wo,
    res,
    wup,
    wdn,
    pb,
    rb,
    mx,
    gb,
    db,
    rd,
    sb,
    rs,
    loc,
    qs,
    qr,
    ks,
    kr,
    ys,
    yr,
    ws,
    wr,
    vs,
    vr,
    os,
    orr,
    xs,
    xr,
    hs,
    hr,
    ps,
    pr,
    dsm,
    drm,
    ss,
    sr,
    fs,
    fr,
    gs,
    gr,
):
    sp = lax.axis_index("sp")
    tp = lax.axis_index("tp")
    z, y = sp // NY, sp % NY
    x, c = tp // 2, tp % 2

    def near(dy, dx):
        return (z * NY + (y + dy) % NY, ((x + dx) % NX) * 2 + c)

    partner = (sp, x * 2 + (1 - c))
    above = (((z + 1) % nz) * NY + y, tp)
    below = (((z + nz - 1) % nz) * NY + y, tp)
    others = [(dy, dx) for dy in range(NY) for dx in range(NX) if dy or dx]

    def send(src, dst, ssem, rsem, device):
        return pltpu.make_async_remote_copy(
            src_ref=src,
            dst_ref=dst,
            send_sem=ssem,
            recv_sem=rsem,
            device_id=device,
            device_id_type=MESH,
        )

    def arrive(ref, ssem, rsem):
        send(ref, ref, ssem, rsem, partner).wait_recv()

    def left(ref, ssem, rsem):
        send(ref, ref, ssem, rsem, partner).wait_send()

    barrier = pltpu.get_barrier_semaphore()
    for device in [near(dy, dx) for dy, dx in others] + [partner, above, below]:
        pl.semaphore_signal(barrier, inc=1, device_id=device, device_id_type=MESH)

    fetch = [
        pltpu.make_async_copy(value_a, vraw, loc.at[5]),
        pltpu.make_async_copy(key_a, kv.at[z, 0], loc.at[6]),
        pltpu.make_async_copy(key_b, kv.at[z, 2, pl.ds(0, 64)], loc.at[7]),
        pltpu.make_async_copy(value_b, kv.at[z, 2, pl.ds(64, 64)], loc.at[8]),
        pltpu.make_async_copy(query_a, qa.at[y], loc.at[9]),
        pltpu.make_async_copy(query_b, qb.at[y], loc.at[10]),
    ]
    for copy in fetch:
        copy.start()
    fetch[0].wait()
    kv[z, 1] = vraw[...].astype(F32).T.astype(BF16)
    for copy in fetch[1:]:
        copy.wait()
    pl.semaphore_wait(barrier, len(others) + 3)

    for ch in range(3):
        for way, device in ((0, above), (1, below)):
            send(
                kv.at[z, ch], kv.at[z, ch], ks.at[way, 0, ch], kr.at[way, 0, ch], device
            ).start()
    for d in range(1, NY):
        send(qa.at[y], qa.at[y], qs.at[d - 1, 0], qr.at[d - 1, 0], near(d, 0)).start()
        send(qb.at[y], qb.at[y], qs.at[d - 1, 1], qr.at[d - 1, 1], near(d, 0)).start()

    own = pl.ds(pl.multiple_of(z * ROWS + y * 32, 32), 32)
    mine = pl.ds(pl.multiple_of(y * FB, FB), FB)
    tok = pl.ds(pl.multiple_of(y * ROWS, ROWS), ROWS)
    side_cols = pl.ds(pl.multiple_of(c * (D // 2), D // 2), D // 2)
    ra = pl.ds(pl.multiple_of(x * 128, 128), 128)
    rbw = pl.ds(pl.multiple_of(512 + x * 64, 64), 64)
    locals_ = [
        pltpu.make_async_copy(up.at[:, mine], wup.at[own], loc.at[0]),
        pltpu.make_async_copy(down.at[:, mine], wdn.at[own], loc.at[1]),
        pltpu.make_async_copy(residual.at[:, side_cols], res.at[tok], loc.at[2]),
        pltpu.make_async_copy(out_first, wo.at[ra], loc.at[3]),
        pltpu.make_async_copy(out_second, wo.at[rbw], loc.at[4]),
        pltpu.make_async_copy(gain_a, ga, loc.at[11]),
        pltpu.make_async_copy(gain_b, gbb, loc.at[12]),
        pltpu.make_async_copy(mlp_gain, mgain, loc.at[13]),
        pltpu.make_async_copy(balance_a, bal.at[0], loc.at[14]),
        pltpu.make_async_copy(balance_b, bal.at[1], loc.at[15]),
    ]
    for copy in locals_:
        copy.start()
    for d in range(1, NX):
        send(out_first, wo.at[ra], os.at[d - 1, 0], orr.at[d - 1, 0], near(0, d)).start()
        send(out_second, wo.at[rbw], os.at[d - 1, 1], orr.at[d - 1, 1], near(0, d)).start()

    stats[pl.ds(0, 4)] = jnp.full((4, BLOCK), LOW, F32)
    stats[pl.ds(4, 4)] = jnp.zeros((4, BLOCK), F32)
    acc[...] = jnp.zeros_like(acc)

    half = nz // 2

    def step(k, ch):
        upper = lax.rem(z - (k + 1) + nz, nz)
        lower = lax.rem(z + k + 1, nz)
        ref = kv.at[upper, ch]
        arrive(ref, ks.at[0, k, ch], kr.at[0, k, ch])

        @pl.when(k < half - 1)
        def _():
            send(ref, ref, ks.at[0, k + 1, ch], kr.at[0, k + 1, ch], above).start()
            arrive(kv.at[lower, ch], ks.at[1, k, ch], kr.at[1, k, ch])

        @pl.when(k < half - 2)
        def _():
            low = kv.at[lower, ch]
            send(low, low, ks.at[1, k + 1, ch], kr.at[1, k + 1, ch], below).start()

    def join(parts, axis):
        return parts[0] if len(parts) == 1 else jnp.concatenate(parts, axis=axis)

    def attend(slots, masked):
        keys = (
            join([kv[u, 0] for u in slots], 0),
            join([kv[u, 2].astype(F32).T.astype(BF16) for u in slots], 0),
        )
        values = (
            join([kv[u, 1] for u in slots], 1),
            join([kv[u, 2, pl.ds(64, 64)] for u in slots], 1),
        )
        items = [(i, part) for i in range(4) for part in range(2)]

        def score(i, part):
            return nt(keys[i // 2], qpad[i, pl.ds(part * 256, 256)])

        ahead = [score(*item) for item in items[:2]]
        for t, (i, part) in enumerate(items):
            if t + 2 < len(items):
                ahead.append(score(*items[t + 2]))
            s = ahead[t]
            cols = pl.ds(part * 256, 256)
            lo, hi = SPANS[i]
            if masked:
                kpos = y * ROWS + lax.broadcasted_iota(jnp.int32, s.shape, 0)
                qpos = part * 256 + lax.broadcasted_iota(jnp.int32, s.shape, 1)
                visible = kpos <= qpos
                s = jnp.where(visible, s, LOW)
            old = stats[pl.ds(i, 1), cols]
            new = jnp.maximum(old, jnp.max(s, axis=0, keepdims=True))
            p = jnp.exp2((s - new) * RATES[i])
            if masked:
                p = jnp.where(visible, p, 0.0)
            alpha = jnp.exp2((old - new) * RATES[i])
            stats[pl.ds(i, 1), cols] = new
            stats[pl.ds(4 + i, 1), cols] = stats[pl.ds(4 + i, 1), cols] * alpha + jnp.sum(
                p, axis=0, keepdims=True
            )
            rows = pl.ds(lo, hi - lo)
            acc[rows, cols] = acc[rows, cols] * alpha + jnp.dot(
                values[i // 2], p.astype(BF16), preferred_element_type=F32
            )

    def sides(k):
        upper = lax.rem(z - (k + 1) + nz, nz)
        lower = lax.rem(z + k + 1, nz)
        first = k + 1 <= z
        second = (z + k + 1 >= nz) & (k < half - 1)

        @pl.when(first & second)
        def _():
            attend((upper, lower), False)

        @pl.when(first != second)
        def _():
            attend((jnp.where(first, upper, lower),), False)

    order = (0, 2, 1)
    for ch in order:
        step(0, ch)
    for d in range(1, NY):
        there = (y + NY - d) % NY
        arrive(qa.at[there], qs.at[d - 1, 0], qr.at[d - 1, 0])
        arrive(qb.at[there], qs.at[d - 1, 1], qr.at[d - 1, 1])
    for d in range(1, NY):
        part = pl.ds(pl.multiple_of(((y + d) % NY) * FB, FB), FB)
        send(up.at[:, part], wup.at[own], ys.at[d - 1, 0], yr.at[d - 1, 0], near(d, 0)).start()
        send(down.at[:, part], wdn.at[own], ys.at[d - 1, 1], yr.at[d - 1, 1], near(d, 0)).start()
    for d in range(1, NY):
        send(
            residual.at[:, side_cols], res.at[tok], vs.at[d - 1], vr.at[d - 1], near(d, 0)
        ).start()
    lane = lax.broadcasted_iota(jnp.int32, (ROWS, 128), 1)
    bounds = ((0, 64), (64, 128), (0, 32), (32, 64))
    for j in range(NY):
        rows = pl.ds(j * ROWS, ROWS)
        low = jnp.concatenate([qb[j], qb[j]], axis=0).astype(F32).T
        for i, (start, stop) in enumerate(bounds):
            keep = (lane >= start) & (lane < stop)
            whole = qa[j].astype(F32) if i < 2 else low
            qpad[i, rows] = jnp.where(keep, whole, 0.0).astype(BF16)

    for ch in order:
        step(1, ch)
    attend((z,), True)

    def shard(ref, at, i):
        return ref.at[pl.ds(pl.multiple_of(at * ROWS + (i % 2) * 64, 64), 64)]

    weights = (wup, wup, wdn, wdn)

    def ring(k, _):
        for ch in order:
            step(k, ch)
        sides(k - 2)
        return 0

    lax.fori_loop(2, EARLY, ring, 0)
    for copy in locals_:
        copy.wait()
    for d in range(1, NY):
        rows = pl.ds(pl.multiple_of(z * ROWS + ((y + NY - d) % NY) * 32, 32), 32)
        for i, w in enumerate((wup, wdn)):
            arrive(w.at[rows], ys.at[d - 1, i], yr.at[d - 1, i])
    for i, w in enumerate(weights):
        for way, device in ((0, above), (1, below)):
            ref = shard(w, z, i)
            send(ref, ref, ws.at[way, 0, i], wr.at[way, 0, i], device).start()
    lax.fori_loop(EARLY, half, ring, 0)

    def rest(k, _):
        sides(k)
        return 0

    lax.fori_loop(half - 2, half, rest, 0)

    def turn(k):
        upper = lax.rem(z - (k + 1) + nz, nz)
        lower = lax.rem(z + k + 1, nz)
        for i, w in enumerate(weights):
            ref = shard(w, upper, i)
            arrive(ref, ws.at[0, k, i], wr.at[0, k, i])
            if k < nz // 2 - 1:
                send(ref, ref, ws.at[0, k + 1, i], wr.at[0, k + 1, i], above).start()
                ref = shard(w, lower, i)
                arrive(ref, ws.at[1, k, i], wr.at[1, k, i])
                if k < nz // 2 - 2:
                    send(ref, ref, ws.at[1, k + 1, i], wr.at[1, k + 1, i], below).start()

    turns = list(range(nz // 2))

    def turn_some(count):
        for k in turns[:count]:
            turn(k)
        del turns[:count]

    for j in range(NY):
        xsnd[j] = acc[:, pl.ds(j * ROWS, ROWS)].astype(BF16)
    for d in range(1, NY):
        there = (y + d) % NY
        part = stats.at[:, pl.ds(pl.multiple_of(there * ROWS, ROWS), ROWS)]
        send(xsnd.at[there], xacc.at[y], xs.at[d - 1, 0], xr.at[d - 1, 0], near(d, 0)).start()
        send(part, xstats.at[y], xs.at[d - 1, 1], xr.at[d - 1, 1], near(d, 0)).start()
    xacc[y] = xsnd[y]
    xstats[y] = stats[:, tok]
    turn_some(TURNS[0])
    for d in range(1, NY):
        there = (y + NY - d) % NY
        arrive(xacc.at[there], xs.at[d - 1, 0], xr.at[d - 1, 0])
        arrive(xstats.at[there], xs.at[d - 1, 1], xr.at[d - 1, 1])

    maps = []
    for i in range(4):
        lo, hi = SPANS[i]
        tops = [xstats[j, i : i + 1] for j in range(NY)]
        top = functools.reduce(jnp.maximum, tops)
        shares = [jnp.exp2((t - top) * RATES[i]) for t in tops]
        total = sum(w * xstats[j, 4 + i : 5 + i] for j, w in enumerate(shares))
        maps.append(
            sum(
                xacc[j, pl.ds(lo, hi - lo)].astype(F32) * (w / total)
                for j, w in enumerate(shares)
            )
        )
    for g in range(2):
        mixed = maps[2 * g] - bal[g, 0] * maps[2 * g + 1]
        size = mixed.shape[0]
        power = jnp.mean(mixed * mixed, axis=0, keepdims=True)
        gain = jnp.broadcast_to((ga, gbb)[g][...], (128, size)).T
        normed = mixed * lax.rsqrt(power + EPSILON) * gain * HEAD_SCALE
        hx[y, x, pl.ds(128 * g, size)] = normed.astype(BF16)
    for n, (dy, dx) in enumerate(others):
        send(hx.at[y, x], hx.at[y, x], hs.at[n], hr.at[n], near(dy, dx)).start()
    turn_some(TURNS[1])
    for d in range(1, NX):
        there = (x + NX - d) % NX
        for i, (size, base) in enumerate(((128, 0), (64, 512))):
            ref = wo.at[pl.ds(pl.multiple_of(base + there * size, size), size)]
            arrive(ref, os.at[d - 1, i], orr.at[d - 1, i])
    for n, (dy, dx) in enumerate(others):
        ref = hx.at[(y + NY - dy) % NY, (x + NX - dx) % NX]
        arrive(ref, hs.at[n], hr.at[n])
    turn_some(1)
    for j in range(NY):
        rows = pl.ds(j * ROWS, ROWS)
        for i in range(NX):
            hmat[rows, pl.ds(i * 128, 128)] = hx[j, i, pl.ds(0, 128)].astype(F32).T.astype(BF16)
        for i in range(NX // 2):
            pair = jnp.concatenate(
                [hx[j, 2 * i, pl.ds(128, 64)], hx[j, 2 * i + 1, pl.ds(128, 64)]], axis=0
            )
            hmat[rows, pl.ds(512 + i * 128, 128)] = pair.astype(F32).T.astype(BF16)

    def block(n):
        return pl.ds(pl.multiple_of(n * FB, FB), FB)

    def project(n, _):
        p = jnp.dot(hmat[...], wo[:, block(n)], preferred_element_type=F32)
        pb[n] = p.astype(BF16)
        send(pb.at[n], rb.at[n], ps.at[n], pr.at[n], partner).start()
        return 0

    def project_own(i, _):
        n = c * (NB // 2) + i
        p = jnp.dot(hmat[...], wo[:, block(n)], preferred_element_type=F32)
        pb[n] = (p + res[:, block(i)].astype(F32)).astype(BF16)
        send(pb.at[n], rb.at[n], ps.at[n], pr.at[n], partner).start()
        return 0

    other = (1 - c) * (NB // 2)
    lax.fori_loop(other, other + NB // 2, project, 0)
    for d in range(1, NY):
        there = pl.ds(pl.multiple_of(((y + NY - d) % NY) * ROWS, ROWS), ROWS)
        arrive(res.at[there], vs.at[d - 1], vr.at[d - 1])
    lax.fori_loop(0, NB // 2, project_own, 0)
    turn_some(1)

    def mix(n, power):
        arrive(rb.at[n], ps.at[n], pr.at[n])
        cols = block(n)
        mixed = (pb[n].astype(F32) + rb[n].astype(F32)).astype(BF16)
        mx[:, cols] = mixed
        wide = mixed.astype(F32)
        gb[:, cols] = (wide * mgain[:, cols]).astype(BF16)
        square = wide * wide
        return power + (square[:, 0:128] + square[:, 128:256])

    power = lax.fori_loop(0, NB, mix, jnp.zeros((BLOCK, 128), F32))
    scale = lax.rsqrt(jnp.sum(power, axis=-1, keepdims=True) * (1.0 / D) + EPSILON)
    turn_some(len(turns))
    lifted = jnp.dot(gb[...], wup[...], preferred_element_type=F32) * scale
    active = jnp.maximum(lifted, 0.0)
    gb[:, pl.ds(0, FB)] = (active * active).astype(BF16)

    def lower_part(n, _):
        rows = pl.ds(pl.multiple_of(n * FB, FB), FB)
        term = nt(gb[:, pl.ds(0, FB)], wdn[rows]).astype(BF16)
        for j in range(NY):
            for h in range(2):
                at = j * ROWS + h * 64
                db[n, h, pl.ds(j * 64, 64)] = term[at : at + 64]
        send(db.at[n, 1 - c], rd.at[n], dsm.at[n], drm.at[n], partner).start()
        return 0

    def gather(n, _):
        arrive(rd.at[n], dsm.at[n], drm.at[n])
        both = (db[n, c].astype(F32) + rd[n].astype(F32)).astype(BF16)
        cols = pl.ds(pl.multiple_of((n % (NB // 2)) * FB, FB), FB)
        for j in range(16):
            sb[n // (NB // 2), j, :, cols] = both[j * 16 : j * 16 + 16]
        return 0

    here = y * NX + x

    def scatter(h):
        for n, (dy, dx) in enumerate(others):
            to = ((y + dy) % NY) * NX + (x + dx) % NX
            send(sb.at[h, to], rs.at[h, here], ss.at[h, n], sr.at[h, n], near(dy, dx)).start()
        rs[h, here] = sb[h, here]

    lax.fori_loop(0, NB - 2, lower_part, 0)
    lax.fori_loop(0, NB // 2, gather, 0)
    scatter(0)
    lax.fori_loop(NB - 2, NB, lower_part, 0)
    lax.fori_loop(NB // 2, NB, gather, 0)
    scatter(1)

    def piece(core, at, h):
        rows = pl.ds(pl.multiple_of(core * 64 + at * 16, 16), 16)
        return out.at[rows, pl.ds(h * (D // 2), D // 2)]

    for h in range(2):
        for n, (dy, dx) in enumerate(others):
            ref = rs.at[h, ((y + NY - dy) % NY) * NX + (x + NX - dx) % NX]
            arrive(ref, ss.at[h, n], sr.at[h, n])

        def final(n, _):
            cols = block(n)
            added = rs[h, :, :, cols].astype(F32).sum(axis=0)
            wide = block(h * (NB // 2) + n)
            base = mx[pl.ds(pl.multiple_of(y * ROWS + c * 64 + x * 16, 16), 16), wide]
            total = (base.astype(F32) + added).astype(BF16)
            out[pl.ds(pl.multiple_of(c * 64 + x * 16, 16), 16), wide] = total
            return 0

        lax.fori_loop(0, NB // 2, final, 0)
        ref = piece(c, x, h)
        for d in range(1, NX):
            send(ref, ref, fs.at[h, d - 1], fr.at[h, d - 1], near(0, d)).start()
        send(ref, ref, gs.at[h, 0], gr.at[h, 0], partner).start()
    for h in range(2):
        for d in range(1, NX):
            ref = piece(c, (x + NX - d) % NX, h)
            arrive(ref, fs.at[h, d - 1], fr.at[h, d - 1])
            send(ref, ref, gs.at[h, d], gr.at[h, d], partner).start()
    for h in range(2):
        for d in range(NX):
            arrive(piece(1 - c, (x + NX - d) % NX, h), gs.at[h, d], gr.at[h, d])

    for d in range(NX - 1):
        for h in range(2):
            left(piece(c, x, h), fs.at[h, d], fr.at[h, d])
        left(out_first, os.at[d, 0], orr.at[d, 0])
        left(out_second, os.at[d, 1], orr.at[d, 1])
    for d in range(NX):
        for h in range(2):
            left(piece(c, x, h), gs.at[h, d], gr.at[h, d])
    for d in range(NY - 1):
        left(qa.at[0], qs.at[d, 0], qr.at[d, 0])
        left(qb.at[0], qs.at[d, 1], qr.at[d, 1])
        left(up.at[:, mine], ys.at[d, 0], yr.at[d, 0])
        left(down.at[:, mine], ys.at[d, 1], yr.at[d, 1])
        left(res.at[tok], vs.at[d], vr.at[d])
        left(xsnd.at[0], xs.at[d, 0], xr.at[d, 0])
        left(xstats.at[0], xs.at[d, 1], xr.at[d, 1])
    for n in range(len(others)):
        left(hx.at[0, 0], hs.at[n], hr.at[n])
        for h in range(2):
            left(sb.at[h, 0], ss.at[h, n], sr.at[h, n])
    for n in range(NB):
        left(pb.at[0], ps.at[n], pr.at[n])
        left(rd.at[0], dsm.at[n], drm.at[n])
    for way, steps in ((0, nz // 2), (1, nz // 2 - 1)):
        for k in range(steps):
            for ch in range(3):
                left(kv.at[0, ch], ks.at[way, k, ch], kr.at[way, k, ch])
            for i in range(4):
                left(shard(wup, 0, 0), ws.at[way, k, i], wr.at[way, k, i])


def layer(
    residual,
    query_first,
    key_first,
    value_first,
    query_second,
    key_second,
    value_second,
    balance_first,
    balance_second,
    head_gain_first,
    head_gain_second,
    out_first,
    out_second,
    mlp_gain,
    up_weight,
    down_weight,
):
    nz = lax.axis_size("sp") // NY
    flat = lambda a: a.reshape(a.shape[0], a.shape[2])
    vmem = pl.BlockSpec(memory_space=pltpu.VMEM)
    anywhere = pl.BlockSpec(memory_space=pl.ANY)
    half = nz // 2
    dma = lambda *shape: pltpu.SemaphoreType.DMA(shape)
    return pl.pallas_call(
        functools.partial(kernel, nz),
        out_shape=jax.ShapeDtypeStruct((ROWS, D), BF16),
        in_specs=[anywhere] * 16,
        out_specs=vmem,
        scratch_shapes=[
            pltpu.VMEM((NY, ROWS, 128), BF16),
            pltpu.VMEM((NY, 64, 128), BF16),
            pltpu.VMEM((ROWS, 128), BF16),
            pltpu.VMEM((1, 128), F32),
            pltpu.VMEM((1, 64), F32),
            pltpu.SMEM((2, 1), F32),
            pltpu.VMEM((1, D), F32),
            pltpu.VMEM((4, BLOCK, 128), BF16),
            pltpu.VMEM((nz, 3, ROWS, 128), BF16),
            pltpu.VMEM((384, BLOCK), F32),
            pltpu.VMEM((8, BLOCK), F32),
            pltpu.VMEM((NY, 384, ROWS), BF16),
            pltpu.VMEM((NY, 384, ROWS), BF16),
            pltpu.VMEM((NY, 8, ROWS), F32),
            pltpu.VMEM((NY, NX, 192, ROWS), BF16),
            pltpu.VMEM((BLOCK, 768), BF16),
            pltpu.VMEM((768, D), BF16),
            pltpu.VMEM((BLOCK, D // 2), BF16),
            pltpu.VMEM((nz * ROWS, FB), BF16),
            pltpu.VMEM((nz * ROWS, FB), BF16),
            pltpu.VMEM((NB, BLOCK, FB), BF16),
            pltpu.VMEM((NB, BLOCK, FB), BF16),
            pltpu.VMEM((BLOCK, D), BF16),
            pltpu.VMEM((BLOCK, D), BF16),
            pltpu.VMEM((NB, 2, BLOCK // 2, FB), BF16),
            pltpu.VMEM((NB, BLOCK // 2, FB), BF16),
            pltpu.VMEM((2, 16, 16, D // 2), BF16),
            pltpu.VMEM((2, 16, 16, D // 2), BF16),
            dma(16),
            dma(3, 2),
            dma(3, 2),
            dma(2, half, 3),
            dma(2, half, 3),
            dma(3, 2),
            dma(3, 2),
            dma(2, half, 4),
            dma(2, half, 4),
            dma(3),
            dma(3),
            dma(3, 2),
            dma(3, 2),
            dma(3, 2),
            dma(3, 2),
            dma(15),
            dma(15),
            dma(NB),
            dma(NB),
            dma(NB),
            dma(NB),
            dma(2, 15),
            dma(2, 15),
            dma(2, 3),
            dma(2, 3),
            dma(2, 4),
            dma(2, 4),
        ],
        compiler_params=pltpu.CompilerParams(
            collective_id=0, has_side_effects=True, vmem_limit_bytes=60 * 1024 * 1024
        ),
    )(
        balance_first,
        balance_second,
        flat(query_first),
        flat(key_first),
        flat(value_first),
        flat(query_second).T,
        flat(key_second).T,
        flat(value_second).T,
        head_gain_first.reshape(1, -1),
        head_gain_second.reshape(1, -1),
        mlp_gain.reshape(1, D),
        residual,
        out_first,
        out_second,
        up_weight,
        down_weight,
    )


def solution(mesh):
    heads = P("sp", "tp", None)
    whole = P("sp", "tp")
    in_specs = (
        P("sp", None),
        *([heads] * 6),
        P("tp"),
        P("tp"),
        P(),
        P(),
        P("tp", None),
        P("tp", None),
        P(),
        whole,
        whole,
    )
    return jax.shard_map(
        layer, mesh=mesh, in_specs=in_specs, out_specs=P("sp", None), check_vma=False
    )
```

```python
import functools
import math

import jax
import jax.numpy as jnp
from jax import lax
from jax.experimental import pallas as pl
from jax.experimental.pallas import tpu as pltpu
from jax.sharding import PartitionSpec as P

MESH = pl.DeviceIdType.MESH
DK_A = 64
DK_B = 32
EPSILON = 1e-06
HEAD_SCALE = 0.8
NY = 4
NX = 4
ROWS = 128
BLOCK = NY * ROWS
D = 2048
FB = 256
NB = D // FB
LOW = -1e30
EARLY = 2
TURNS = (4, 6, 0, 1)
QN = 4
QB = NB // QN
QW = D // QN
RATES = tuple(k**-0.5 * math.log2(math.e) for k in (DK_A, DK_A, DK_B, DK_B))
SPANS = ((0, 128), (128, 256), (256, 320), (320, 384))
F32 = jnp.float32
BF16 = jnp.bfloat16


def nt(a, b):
    return lax.dot_general(a, b, (((1,), (1,)), ((), ())), preferred_element_type=F32)


def kernel(
    nz,
    balance_a,
    balance_b,
    query_a,
    key_a,
    value_a,
    query_b,
    key_b,
    value_b,
    gain_a,
    gain_b,
    mlp_gain,
    residual,
    out_first,
    out_second,
    up,
    down,
    out,
    qa,
    qb,
    vraw,
    ga,
    gbb,
    bal,
    mgain,
    qpad,
    kv,
    acc,
    stats,
    xsnd,
    xacc,
    xstats,
    hx,
    hmat,
    wo,
    res,
    wt,
    pb,
    rb,
    mx,
    gb,
    db,
    rd,
    sb,
    rs,
    loc,
    qs,
    qr,
    ks,
    kr,
    ys,
    yr,
    ws,
    wr,
    vs,
    vr,
    os,
    orr,
    xs,
    xr,
    hs,
    hr,
    ps,
    pr,
    dsm,
    drm,
    ss,
    sr,
    fs,
    fr,
    gs,
    gr,
):
    sp = lax.axis_index("sp")
    tp = lax.axis_index("tp")
    z, y = sp // NY, sp % NY
    x, c = tp // 2, tp % 2

    def near(dy, dx):
        return (z * NY + (y + dy) % NY, ((x + dx) % NX) * 2 + c)

    partner = (sp, x * 2 + (1 - c))
    above = (((z + 1) % nz) * NY + y, tp)
    below = (((z + nz - 1) % nz) * NY + y, tp)
    others = [(dy, dx) for dy in range(NY) for dx in range(NX) if dy or dx]

    def send(src, dst, ssem, rsem, device):
        return pltpu.make_async_remote_copy(
            src_ref=src,
            dst_ref=dst,
            send_sem=ssem,
            recv_sem=rsem,
            device_id=device,
            device_id_type=MESH,
        )

    def arrive(ref, ssem, rsem):
        send(ref, ref, ssem, rsem, partner).wait_recv()

    def left(ref, ssem, rsem):
        send(ref, ref, ssem, rsem, partner).wait_send()

    barrier = pltpu.get_barrier_semaphore()
    for device in [near(dy, dx) for dy, dx in others] + [partner, above, below]:
        pl.semaphore_signal(barrier, inc=1, device_id=device, device_id_type=MESH)

    fetch = [
        pltpu.make_async_copy(value_a, vraw, loc.at[5]),
        pltpu.make_async_copy(key_a, kv.at[z, 0], loc.at[6]),
        pltpu.make_async_copy(key_b, kv.at[z, 2, pl.ds(0, 64)], loc.at[7]),
        pltpu.make_async_copy(value_b, kv.at[z, 2, pl.ds(64, 64)], loc.at[8]),
        pltpu.make_async_copy(query_a, qa.at[y], loc.at[9]),
        pltpu.make_async_copy(query_b, qb.at[y], loc.at[10]),
    ]
    for copy in fetch:
        copy.start()
    fetch[0].wait()
    kv[z, 1] = vraw[...].astype(F32).T.astype(BF16)
    for copy in fetch[1:]:
        copy.wait()
    pl.semaphore_wait(barrier, len(others) + 3)

    for ch in range(3):
        for way, device in ((0, above), (1, below)):
            send(
                kv.at[z, ch], kv.at[z, ch], ks, kr.at[way, 0, ch], device
            ).start()
    for d in range(1, NY):
        send(qa.at[y], qa.at[y], qs.at[d - 1, 0], qr.at[d - 1, 0], near(d, 0)).start()
        send(qb.at[y], qb.at[y], qs.at[d - 1, 1], qr.at[d - 1, 1], near(d, 0)).start()

    own = pl.ds(pl.multiple_of(z * ROWS + y * 32, 32), 32)
    mine = pl.ds(pl.multiple_of(y * FB, FB), FB)
    tok = pl.ds(pl.multiple_of(y * ROWS, ROWS), ROWS)
    side_cols = pl.ds(pl.multiple_of(c * (D // 2), D // 2), D // 2)
    ra = pl.ds(pl.multiple_of(x * 128, 128), 128)
    rbw = pl.ds(pl.multiple_of(512 + x * 64, 64), 64)
    locals_ = [
        pltpu.make_async_copy(up.at[:, mine], wt.at[0, own], loc.at[0]),
        pltpu.make_async_copy(down.at[:, mine], wt.at[1, own], loc.at[1]),
        pltpu.make_async_copy(residual.at[:, side_cols], res.at[tok], loc.at[2]),
        pltpu.make_async_copy(out_first, wo.at[ra], loc.at[3]),
        pltpu.make_async_copy(out_second, wo.at[rbw], loc.at[4]),
        pltpu.make_async_copy(gain_a, ga, loc.at[11]),
        pltpu.make_async_copy(gain_b, gbb, loc.at[12]),
        pltpu.make_async_copy(mlp_gain, mgain, loc.at[13]),
        pltpu.make_async_copy(balance_a, bal.at[0], loc.at[14]),
        pltpu.make_async_copy(balance_b, bal.at[1], loc.at[15]),
    ]
    for copy in locals_:
        copy.start()
    for d in range(1, NX):
        send(out_first, wo.at[ra], os.at[d - 1, 0], orr.at[d - 1, 0], near(0, d)).start()
        send(out_second, wo.at[rbw], os.at[d - 1, 1], orr.at[d - 1, 1], near(0, d)).start()

    stats[pl.ds(0, 4)] = jnp.full((4, BLOCK), LOW, F32)
    stats[pl.ds(4, 4)] = jnp.zeros((4, BLOCK), F32)
    acc[...] = jnp.zeros_like(acc)

    half = nz // 2

    def step(k, ch):
        upper = lax.rem(z - (k + 1) + nz, nz)
        lower = lax.rem(z + k + 1, nz)
        ref = kv.at[upper, ch]
        arrive(ref, ks, kr.at[0, k, ch])

        @pl.when(k < half - 1)
        def _():
            send(ref, ref, ks, kr.at[0, k + 1, ch], above).start()
            arrive(kv.at[lower, ch], ks, kr.at[1, k, ch])

        @pl.when(k < half - 2)
        def _():
            low = kv.at[lower, ch]
            send(low, low, ks, kr.at[1, k + 1, ch], below).start()

    def join(parts, axis):
        return parts[0] if len(parts) == 1 else jnp.concatenate(parts, axis=axis)

    def attend(slots, masked):
        keys = (
            join([kv[u, 0] for u in slots], 0),
            join([kv[u, 2].astype(F32).T.astype(BF16) for u in slots], 0),
        )
        values = (
            join([kv[u, 1] for u in slots], 1),
            join([kv[u, 2, pl.ds(64, 64)] for u in slots], 1),
        )
        items = [(i, part) for i in range(4) for part in range(2)]

        def score(i, part):
            return nt(keys[i // 2], qpad[i, pl.ds(part * 256, 256)])

        ahead = [score(*item) for item in items[:2]]
        for t, (i, part) in enumerate(items):
            if t + 2 < len(items):
                ahead.append(score(*items[t + 2]))
            s = ahead[t]
            cols = pl.ds(part * 256, 256)
            lo, hi = SPANS[i]
            if masked:
                kpos = y * ROWS + lax.broadcasted_iota(jnp.int32, s.shape, 0)
                qpos = part * 256 + lax.broadcasted_iota(jnp.int32, s.shape, 1)
                visible = kpos <= qpos
                s = jnp.where(visible, s, LOW)
            old = stats[pl.ds(i, 1), cols]
            new = jnp.maximum(old, jnp.max(s, axis=0, keepdims=True))
            p = jnp.exp2((s - new) * RATES[i])
            if masked:
                p = jnp.where(visible, p, 0.0)
            alpha = jnp.exp2((old - new) * RATES[i])
            stats[pl.ds(i, 1), cols] = new
            stats[pl.ds(4 + i, 1), cols] = stats[pl.ds(4 + i, 1), cols] * alpha + jnp.sum(
                p, axis=0, keepdims=True
            )
            rows = pl.ds(lo, hi - lo)
            acc[rows, cols] = acc[rows, cols] * alpha + jnp.dot(
                values[i // 2], p.astype(BF16), preferred_element_type=F32
            )

    def sides(k):
        upper = lax.rem(z - (k + 1) + nz, nz)
        lower = lax.rem(z + k + 1, nz)
        first = k + 1 <= z
        second = (z + k + 1 >= nz) & (k < half - 1)

        @pl.when(first & second)
        def _():
            attend((upper, lower), False)

        @pl.when(first != second)
        def _():
            attend((jnp.where(first, upper, lower),), False)

    order = (0, 2, 1)
    for ch in order:
        step(0, ch)
    for d in range(1, NY):
        there = (y + NY - d) % NY
        arrive(qa.at[there], qs.at[d - 1, 0], qr.at[d - 1, 0])
        arrive(qb.at[there], qs.at[d - 1, 1], qr.at[d - 1, 1])
    for d in range(1, NY):
        part = pl.ds(pl.multiple_of(((y + d) % NY) * FB, FB), FB)
        send(up.at[:, part], wt.at[0, own], ys.at[d - 1, 0], yr.at[d - 1, 0], near(d, 0)).start()
        send(down.at[:, part], wt.at[1, own], ys.at[d - 1, 1], yr.at[d - 1, 1], near(d, 0)).start()
    for d in range(1, NY):
        send(
            residual.at[:, side_cols], res.at[tok], vs.at[d - 1], vr.at[d - 1], near(d, 0)
        ).start()
    lane = lax.broadcasted_iota(jnp.int32, (ROWS, 128), 1)
    bounds = ((0, 64), (64, 128), (0, 32), (32, 64))
    for j in range(NY):
        rows = pl.ds(j * ROWS, ROWS)
        low = jnp.concatenate([qb[j], qb[j]], axis=0).astype(F32).T
        for i, (start, stop) in enumerate(bounds):
            keep = (lane >= start) & (lane < stop)
            whole = qa[j].astype(F32) if i < 2 else low
            qpad[i, rows] = jnp.where(keep, whole, 0.0).astype(BF16)

    for ch in order:
        step(1, ch)
    attend((z,), True)

    def shard(at, i, h):
        return wt.at[i, pl.ds(pl.multiple_of(at * ROWS + h * 64, 64), 64)]

    def half_turn(w):
        k, i = w // 2, w % 2
        upper = lax.rem(z - (k + 1) + nz, nz)
        lower = lax.rem(z + k + 1, nz)
        for h in range(2):
            n = i * 2 + h
            ref = shard(upper, i, h)
            low = shard(lower, i, h)
            arrive(ref, ws.at[i], wr.at[0, k, n])

            def onward(ref=ref, low=low, n=n):
                send(ref, ref, ws.at[i], wr.at[0, k + 1, n], above).start()
                arrive(low, ws.at[i], wr.at[1, k, n])

            def downward(low=low, n=n):
                send(low, low, ws.at[i], wr.at[1, k + 1, n], below).start()

            if isinstance(w, int):
                if k < half - 1:
                    onward()
                if k < half - 2:
                    downward()
            else:
                pl.when(k < half - 1)(onward)
                pl.when(k < half - 2)(downward)

    def ring(k, _):
        for ch in order:
            step(k, ch)
        sides(k - 2)

        @pl.when(k > EARLY)
        def _():
            half_turn(k - EARLY - 1)

        return 0

    for copy in locals_:
        copy.wait()
    for d in range(1, NY):
        rows = pl.ds(pl.multiple_of(z * ROWS + ((y + NY - d) % NY) * 32, 32), 32)
        for i in range(2):
            arrive(wt.at[i, rows], ys.at[d - 1, i], yr.at[d - 1, i])
    for i in range(2):
        for h in range(2):
            for way, device in ((0, above), (1, below)):
                ref = shard(z, i, h)
                n = i * 2 + h
                send(ref, ref, ws.at[n // 2], wr.at[way, 0, n], device).start()
    lax.fori_loop(2, half, ring, 0)

    def rest(k, _):
        sides(k)
        return 0

    lax.fori_loop(half - 2, half, rest, 0)

    turns = list(range(half - EARLY - 1, 2 * half))

    def turn_some(count):
        for k in turns[:count]:
            half_turn(k)
        del turns[:count]

    for j in range(NY):
        xsnd[j] = acc[:, pl.ds(j * ROWS, ROWS)].astype(BF16)
    for d in range(1, NY):
        there = (y + d) % NY
        part = stats.at[:, pl.ds(pl.multiple_of(there * ROWS, ROWS), ROWS)]
        send(xsnd.at[there], xacc.at[y], xs.at[d - 1, 0], xr.at[d - 1, 0], near(d, 0)).start()
        send(part, xstats.at[y], xs.at[d - 1, 1], xr.at[d - 1, 1], near(d, 0)).start()
    xacc[y] = xsnd[y]
    xstats[y] = stats[:, tok]
    turn_some(TURNS[0])
    for d in range(1, NY):
        there = (y + NY - d) % NY
        arrive(xacc.at[there], xs.at[d - 1, 0], xr.at[d - 1, 0])
        arrive(xstats.at[there], xs.at[d - 1, 1], xr.at[d - 1, 1])

    maps = []
    for i in range(4):
        lo, hi = SPANS[i]
        tops = [xstats[j, i : i + 1] for j in range(NY)]
        top = functools.reduce(jnp.maximum, tops)
        shares = [jnp.exp2((t - top) * RATES[i]) for t in tops]
        total = sum(w * xstats[j, 4 + i : 5 + i] for j, w in enumerate(shares))
        maps.append(
            sum(
                xacc[j, pl.ds(lo, hi - lo)].astype(F32) * (w / total)
                for j, w in enumerate(shares)
            )
        )
    for g in range(2):
        mixed = maps[2 * g] - bal[g, 0] * maps[2 * g + 1]
        size = mixed.shape[0]
        power = jnp.mean(mixed * mixed, axis=0, keepdims=True)
        gain = jnp.broadcast_to((ga, gbb)[g][...], (128, size)).T
        normed = mixed * lax.rsqrt(power + EPSILON) * gain * HEAD_SCALE
        hx[y, x, pl.ds(128 * g, size)] = normed.astype(BF16)
    for n, (dy, dx) in enumerate(others):
        send(hx.at[y, x], hx.at[y, x], hs, hr, near(dy, dx)).start()
    turn_some(TURNS[1])
    for d in range(1, NX):
        there = (x + NX - d) % NX
        for i, (size, base) in enumerate(((128, 0), (64, 512))):
            ref = wo.at[pl.ds(pl.multiple_of(base + there * size, size), size)]
            arrive(ref, os.at[d - 1, i], orr.at[d - 1, i])
    arrive(hmat.at[pl.ds(0, 480)], hs, hr)
    turn_some(TURNS[2])
    for j in range(NY):
        rows = pl.ds(j * ROWS, ROWS)
        for i in range(NX):
            hmat[rows, pl.ds(i * 128, 128)] = hx[j, i, pl.ds(0, 128)].astype(F32).T.astype(BF16)
        for i in range(NX // 2):
            pair = jnp.concatenate(
                [hx[j, 2 * i, pl.ds(128, 64)], hx[j, 2 * i + 1, pl.ds(128, 64)]], axis=0
            )
            hmat[rows, pl.ds(512 + i * 128, 128)] = pair.astype(F32).T.astype(BF16)

    def block(n):
        return pl.ds(pl.multiple_of(n * FB, FB), FB)

    def project(n, _):
        p = jnp.dot(hmat[...], wo[:, block(n)], preferred_element_type=F32)
        pb[n] = p.astype(BF16)
        send(pb.at[n], rb.at[n], ps, pr.at[n], partner).start()
        return 0

    def project_own(i, _):
        n = c * (NB // 2) + i
        p = jnp.dot(hmat[...], wo[:, block(n)], preferred_element_type=F32)
        pb[n] = (p + res[:, block(i)].astype(F32)).astype(BF16)
        send(pb.at[n], rb.at[n], ps, pr.at[n], partner).start()
        return 0

    other = (1 - c) * (NB // 2)
    lax.fori_loop(other, other + NB // 2, project, 0)
    for d in range(1, NY):
        there = pl.ds(pl.multiple_of(((y + NY - d) % NY) * ROWS, ROWS), ROWS)
        arrive(res.at[there], vs.at[d - 1], vr.at[d - 1])
    lax.fori_loop(0, NB // 2, project_own, 0)
    turn_some(TURNS[3])

    def mix(n, power):
        arrive(rb.at[n], ps, pr.at[n])
        cols = block(n)
        mixed = (pb[n].astype(F32) + rb[n].astype(F32)).astype(BF16)
        mx[:, cols] = mixed
        wide = mixed.astype(F32)
        gb[:, cols] = (wide * mgain[:, cols]).astype(BF16)
        square = wide * wide
        return power + (square[:, 0:128] + square[:, 128:256])

    power = lax.fori_loop(0, NB, mix, jnp.zeros((BLOCK, 128), F32))
    scale = lax.rsqrt(jnp.sum(power, axis=-1, keepdims=True) * (1.0 / D) + EPSILON)
    turn_some(len(turns))
    lifted = jnp.dot(gb[...], wt[0], preferred_element_type=F32) * scale
    active = jnp.maximum(lifted, 0.0)
    gb[:, pl.ds(0, FB)] = (active * active).astype(BF16)

    def lower_part(n, _):
        rows = pl.ds(pl.multiple_of(n * FB, FB), FB)
        term = nt(gb[:, pl.ds(0, FB)], wt[1, rows]).astype(BF16)
        for j in range(NY):
            for h in range(2):
                at = j * ROWS + h * 64
                db[n, h, pl.ds(j * 64, 64)] = term[at : at + 64]
        send(db.at[n, 1 - c], rd.at[n], dsm, drm.at[n], partner).start()
        return 0

    def gather(n, _):
        arrive(rd.at[n], dsm, drm.at[n])
        both = (db[n, c].astype(F32) + rd[n].astype(F32)).astype(BF16)
        cols = pl.ds(pl.multiple_of((n % QB) * FB, FB), FB)
        for j in range(16):
            sb[n // QB, j, :, cols] = both[j * 16 : j * 16 + 16]
        return 0

    here = y * NX + x

    def scatter(h):
        for n, (dy, dx) in enumerate(others):
            to = ((y + dy) % NY) * NX + (x + dx) % NX
            send(sb.at[h, to], rs.at[h, here], ss, sr.at[h], near(dy, dx)).start()
        rs[h, here] = sb[h, here]

    lax.fori_loop(0, QB, lower_part, 0)
    for h in range(QN):
        if h + 1 < QN:
            lax.fori_loop((h + 1) * QB, (h + 2) * QB, lower_part, 0)
        lax.fori_loop(h * QB, (h + 1) * QB, gather, 0)
        scatter(h)

    for d in range(NY - 1):
        left(qa.at[0], qs.at[d, 0], qr.at[d, 0])
        left(qb.at[0], qs.at[d, 1], qr.at[d, 1])
        left(up.at[:, mine], ys.at[d, 0], yr.at[d, 0])
        left(down.at[:, mine], ys.at[d, 1], yr.at[d, 1])
        left(res.at[tok], vs.at[d], vr.at[d])
        left(xsnd.at[0], xs.at[d, 0], xr.at[d, 0])
        left(xstats.at[0], xs.at[d, 1], xr.at[d, 1])
    left(hmat.at[pl.ds(0, 480)], hs, hr)
    left(pb, ps, pr.at[0])
    left(rd, dsm, drm.at[0])
    left(kv.at[pl.ds(0, nz - 1)], ks, kr.at[0, 0, 0])
    for i in range(2):
        left(wt.at[i, pl.ds(0, (nz - 1) * ROWS)], ws.at[i], wr.at[0, 0, 0])
    for d in range(NX - 1):
        left(out_first, os.at[d, 0], orr.at[d, 0])
        left(out_second, os.at[d, 1], orr.at[d, 1])

    def piece(core, at, h):
        rows = pl.ds(pl.multiple_of(core * 64 + at * 16, 16), 16)
        return out.at[rows, pl.ds(h * QW, QW)]

    for h in range(QN):
        arrive(rs.at[h, pl.ds(0, 15)], ss, sr.at[h])

        def final(n, _):
            cols = block(n)
            added = rs[h, :, :, cols].astype(F32).sum(axis=0)
            wide = block(h * QB + n)
            base = mx[pl.ds(pl.multiple_of(y * ROWS + c * 64 + x * 16, 16), 16), wide]
            total = (base.astype(F32) + added).astype(BF16)
            out[pl.ds(pl.multiple_of(c * 64 + x * 16, 16), 16), wide] = total
            return 0

        lax.fori_loop(0, QB, final, 0)
        ref = piece(c, x, h)
        for d in range(1, NX):
            send(ref, ref, fs, fr.at[h], near(0, d)).start()
        send(ref, ref, gs, gr, partner).start()
    for h in range(QN):
        arrive(rs.at[h, pl.ds(0, 3)], fs, fr.at[h])
        for d in range(1, NX):
            ref = piece(c, (x + NX - d) % NX, h)
            send(ref, ref, gs, gr, partner).start()
    arrive(out.at[pl.ds(0, 64)], gs, gr)
    left(out.at[pl.ds(0, 64)], gs, gr)
    left(out.at[pl.ds(0, 48)], fs, fr.at[0])
    left(sb.at[:, pl.ds(0, 15)], ss, sr.at[0])


def layer(
    residual,
    query_first,
    key_first,
    value_first,
    query_second,
    key_second,
    value_second,
    balance_first,
    balance_second,
    head_gain_first,
    head_gain_second,
    out_first,
    out_second,
    mlp_gain,
    up_weight,
    down_weight,
):
    nz = lax.axis_size("sp") // NY
    flat = lambda a: a.reshape(a.shape[0], a.shape[2])
    vmem = pl.BlockSpec(memory_space=pltpu.VMEM)
    anywhere = pl.BlockSpec(memory_space=pl.ANY)
    half = nz // 2
    dma = lambda *shape: pltpu.SemaphoreType.DMA(shape)
    return pl.pallas_call(
        functools.partial(kernel, nz),
        out_shape=jax.ShapeDtypeStruct((ROWS, D), BF16),
        in_specs=[anywhere] * 16,
        out_specs=vmem,
        scratch_shapes=[
            pltpu.VMEM((NY, ROWS, 128), BF16),
            pltpu.VMEM((NY, 64, 128), BF16),
            pltpu.VMEM((ROWS, 128), BF16),
            pltpu.VMEM((1, 128), F32),
            pltpu.VMEM((1, 64), F32),
            pltpu.SMEM((2, 1), F32),
            pltpu.VMEM((1, D), F32),
            pltpu.VMEM((4, BLOCK, 128), BF16),
            pltpu.VMEM((nz, 3, ROWS, 128), BF16),
            pltpu.VMEM((384, BLOCK), F32),
            pltpu.VMEM((8, BLOCK), F32),
            pltpu.VMEM((NY, 384, ROWS), BF16),
            pltpu.VMEM((NY, 384, ROWS), BF16),
            pltpu.VMEM((NY, 8, ROWS), F32),
            pltpu.VMEM((NY, NX, 192, ROWS), BF16),
            pltpu.VMEM((BLOCK, 768), BF16),
            pltpu.VMEM((768, D), BF16),
            pltpu.VMEM((BLOCK, D // 2), BF16),
            pltpu.VMEM((2, nz * ROWS, FB), BF16),
            pltpu.VMEM((NB, BLOCK, FB), BF16),
            pltpu.VMEM((NB, BLOCK, FB), BF16),
            pltpu.VMEM((BLOCK, D), BF16),
            pltpu.VMEM((BLOCK, D), BF16),
            pltpu.VMEM((NB, 2, BLOCK // 2, FB), BF16),
            pltpu.VMEM((NB, BLOCK // 2, FB), BF16),
            pltpu.VMEM((QN, 16, 16, QW), BF16),
            pltpu.VMEM((QN, 16, 16, QW), BF16),
            dma(16),
            dma(3, 2),
            dma(3, 2),
            pltpu.SemaphoreType.DMA,
            dma(2, half, 3),
            dma(3, 2),
            dma(3, 2),
            dma(2),
            dma(2, half, 4),
            dma(3),
            dma(3),
            dma(3, 2),
            dma(3, 2),
            dma(3, 2),
            dma(3, 2),
            pltpu.SemaphoreType.DMA,
            pltpu.SemaphoreType.DMA,
            pltpu.SemaphoreType.DMA,
            dma(NB),
            pltpu.SemaphoreType.DMA,
            dma(NB),
            pltpu.SemaphoreType.DMA,
            dma(QN),
            pltpu.SemaphoreType.DMA,
            dma(QN),
            pltpu.SemaphoreType.DMA,
            pltpu.SemaphoreType.DMA,
        ],
        compiler_params=pltpu.CompilerParams(
            collective_id=0, has_side_effects=True, vmem_limit_bytes=60 * 1024 * 1024
        ),
    )(
        balance_first,
        balance_second,
        flat(query_first),
        flat(key_first),
        flat(value_first),
        flat(query_second).T,
        flat(key_second).T,
        flat(value_second).T,
        head_gain_first.reshape(1, -1),
        head_gain_second.reshape(1, -1),
        mlp_gain.reshape(1, D),
        residual,
        out_first,
        out_second,
        up_weight,
        down_weight,
    )


def solution(mesh):
    heads = P("sp", "tp", None)
    whole = P("sp", "tp")
    in_specs = (
        P("sp", None),
        *([heads] * 6),
        P("tp"),
        P("tp"),
        P(),
        P(),
        P("tp", None),
        P("tp", None),
        P(),
        whole,
        whole,
    )
    return jax.shard_map(
        layer, mesh=mesh, in_specs=in_specs, out_specs=P("sp", None), check_vma=False
    )
```
